256 devices in a mesh: ep: 64 (over z, x, core), tp: 4 (over y).
Axes of the slice: x: 4, y: 4, z: 8, core: 2. Of those that a mesh axis runs over, the one named last changes fastest.
Arguments:
- queries: bfloat16 [32768, 1024], P('ep', 'tp'), may hold values from -6 to 6
- mixer_key_rows: bfloat16 [32768, 1024], P('ep', 'tp'), may hold values from -6 to 6
- mixer_value_rows: bfloat16 [32768, 2048], P('ep', 'tp'), may hold values from -6 to 6
- log_input_gate: float32 [8, 32768], P('tp', 'ep'), may hold values from -6 to 136
- forget_gate_logits: float32 [8, 32768], P('tp', 'ep'), may hold values from 1 to 20
- extra_log_decay: float32 [8, 32768], P('tp', 'ep'), may hold values from -1.4 to 0
- head_norm_gain: float32 [2048], P('tp'), may hold values from 0.1 to 1.9
- mixer_output_weight: bfloat16 [2048, 2048], P('tp'), may hold values from -0.125 to 0.125
- expert_input_rows: bfloat16 [16384, 2048], P(('ep', 'tp')), may hold values from -6 to 6
- expert_norm_gain: float32 [2048], replicated, may hold values from 0.1 to 1.9
- routes: int32 [16384, 3], P(('ep', 'tp')), may hold values from 0 to 63, all different within a row; in each aligned block of 64 rows (0 to 63, 64 to 127, ...) at most 6 rows name the same one
- router_picked_scores: float32 [16384, 3], P(('ep', 'tp')), may hold values from 0.1 to 1
- expert_gate_weight: bfloat16 [64, 2048, 1024], P('ep', None, 'tp'), may hold values from -0.125 to 0.125
- expert_up_weight: bfloat16 [64, 2048, 1024], P('ep', None, 'tp'), may hold values from -0.125 to 0.125
- expert_down_weight: bfloat16 [64, 2048, 1024], P('ep', None, 'tp'), may hold values from -0.1875 to 0.1875
Outputs:
- mixer_output: bfloat16 [32768, 2048], P(('ep', 'tp'))
- expert_out: bfloat16 [16384, 2048], P(('ep', 'tp'))
The draws below stay inside these ranges and needn't reach their ends.
Inputs may be any that keep to these rules, and one draw needn't show every extreme that they name: `routes`: in each aligned block of 64 rows, the rows of one device, no expert is named by more than 6 rows, a bound that some block reaches; a row names 3 different experts.
All inputs are finite; a program needn't handle non-finite values.
Results may differ from the reference program's by a relative error of at most 0.014.
Values may be sent and summed in bfloat16 or wider, within the bound.
No kernel may reach another device: no remote copies, remote signals or barrier semaphores. Data moves between devices by JAX's collectives and lax.ppermute only.
A program may use at most 128 MiB of HBM per device.

```python
import math
import jax
import jax.numpy as jnp
import numpy as np
from jax import lax

D = 2048
HEADS = 8
KEY_DIM = 128
VALUE_DIM = 256
BLOCK = 64
EXPERT_HIDDEN = 1024
TOPK = 3
MIX_TOK = 512
MOE_TOK = 64
EXPERTS = 64
CAP = 6
SEQ = 32768
MOE_TOKENS = 16384
N_EP = 64
N_TP = 4


def draw_log_input_gate(key, part):
    first = jax.random.fold_in(jax.random.fold_in(key, 11), 0)
    values = 1.5 * jnp.clip(jax.random.normal(first, (HEADS, SEQ), jnp.float32), -4.0, 4.0)
    return values


def draw_forget_gate_logits(key, part):
    first, second, third = jax.random.split(jax.random.fold_in(key, 23), 3)
    order = jax.random.permutation(first, HEADS)
    quick_heads = order < HEADS // 2
    segment_count = SEQ // MIX_TOK
    factor = jax.random.uniform(second, (HEADS, segment_count), jnp.float32, 0.0, math.log(4.0))
    factor = jnp.repeat(factor, MIX_TOK, axis=1)
    noise = 0.7 * jnp.clip(jax.random.normal(third, (HEADS, SEQ), jnp.float32), -3.0, 3.0)
    slow_values = math.log(2.0 * SEQ) + factor + noise
    quick_values = math.log(40.0) + noise
    return jnp.where(quick_heads[:, None], quick_values, slow_values)


def draw_extra_log_decay(key, part):
    first, second = jax.random.split(jax.random.fold_in(key, 37), 2)
    places = jax.random.randint(first, (HEADS, 2), 0, SEQ)
    losses = jax.random.uniform(second, (HEADS, 2), jnp.float32, 0.22, 0.69)
    head_rows = jnp.broadcast_to(jnp.arange(HEADS, dtype=jnp.int32)[:, None], (HEADS, 2))
    return jnp.zeros((HEADS, SEQ), jnp.float32).at[head_rows, places].add(-losses)


def shard_levels(rng, dims, cuts, low, high):
    factor_of, own = 1.0, jax.random.fold_in(rng, 6)
    for dim, parts in cuts:
        heights = jnp.exp(jax.random.uniform(jax.random.fold_in(own, dim), (parts,), jnp.float32, low / len(cuts), high / len(cuts)))
        factor_of = factor_of * jnp.repeat(heights, dims[dim] // parts).reshape([-1 if axis == dim else 1 for axis in range(len(dims))])
    return factor_of


def assign_block(own_key, own, number, rows, count, top, bound, skew):
    order = jax.random.permutation(own_key, count)
    crowded, ordinary = load_shares(count, rows * top, bound, skew, True), load_shares(count, rows * top, bound, skew, False)
    places = jnp.arange(count)

    def named(tallies, offset_by):
        used = int((tallies > 0).sum())
        fixed = max(1, used // 4)
        shifted = fixed + (places - fixed + offset_by * (used - fixed)) % max(1, count - fixed)
        return jnp.zeros((count,), jnp.int32).at[order[jnp.where(places < fixed, places, shifted)]].set(jnp.asarray(tallies, jnp.int32))

    tallies = jnp.where(number % 4 == 0, named(crowded, number // 4), named(ordinary, number - number // 4 - 1))
    mixed = jax.random.permutation(jax.random.fold_in(own, 3), count)
    source_of, receiver = mixed[0:count // 2 * 2:2], mixed[1:count // 2 * 2:2]
    slack = jnp.minimum(tallies[source_of] - 1, bound - tallies[receiver]) // 2
    slack = jnp.where((source_of == order[0]) | (receiver == order[0]) | (tallies[receiver] == 0), 0, jnp.maximum(slack, 0))
    shifted = jax.random.randint(jax.random.fold_in(own, 4), (count // 2,), 0, 1 << 20) % (slack + 1)
    tallies = tallies.at[source_of].add(-shifted).at[receiver].add(shifted)
    labels = jnp.searchsorted(jnp.cumsum(tallies), jnp.arange(rows * top), side="right").astype(jnp.int32)
    grid = labels.reshape(top, rows).T
    grid = grid[jax.random.permutation(jax.random.fold_in(own, 1), rows)]
    offset_by = jax.random.randint(jax.random.fold_in(own, 2), (rows, 1), 0, top)
    return jnp.take_along_axis(grid, (jnp.arange(top)[None, :] + offset_by) % top, axis=1)


def load_shares(number_of, total, reach, skew, full):
    weights = [(1 << 20) // math.isqrt(rank ** skew) + 1 for rank in range(1, number_of + 1)]
    largest = reach if full else min(reach, max(-(-total // number_of), total * weights[0] // sum(weights)))
    least = 1 if total - largest >= number_of - 1 else 0
    given, surplus = [largest] + [least] * (number_of - 1), total - largest - least * (number_of - 1)
    while surplus > 0:
        free = [i for i in range(1, number_of) if given[i] < largest] or [i for i in range(1, number_of) if given[i] < reach]
        whole, remaining = sum([weights[i] for i in free]), surplus
        for i in free:
            extra = min(reach - given[i], max(1, remaining * weights[i] // whole), surplus)
            given[i] = given[i] + extra
            surplus = surplus - extra
    return np.array(given)


def centred(stream_key, dims, scale, reach, cuts=(), kind=jnp.bfloat16):
    values = jax.random.normal(stream_key, dims, jnp.float32) * scale
    if len(cuts) > 0:
        values = shard_levels(stream_key, dims, cuts, -0.22, 0.18) * values
    return jnp.clip(values, min=-reach, max=reach).astype(kind)


def setup_inputs(seed: int = 0) -> dict:
    streams_of = jax.random.split(jax.random.key(seed), 16)
    queries = centred(streams_of[0], (SEQ, HEADS * KEY_DIM), 1.0, 6.0, ((0, 64), (1, 4)))
    mixer_key_rows = centred(streams_of[1], (SEQ, HEADS * KEY_DIM), 1.0, 6.0, ((0, 64), (1, 4)))
    mixer_value_rows = centred(streams_of[2], (SEQ, HEADS * VALUE_DIM), 1.0, 6.0, ((0, 64), (1, 4)))
    log_input_gate = draw_log_input_gate(jax.random.fold_in(streams_of[15], 71), 0)
    forget_gate_logits = draw_forget_gate_logits(jax.random.fold_in(streams_of[15], 71), 0)
    extra_log_decay = draw_extra_log_decay(jax.random.fold_in(streams_of[15], 71), 0)
    head_norm_gain = jnp.clip(1.0 + 0.18 * jax.random.normal(streams_of[6], (HEADS * VALUE_DIM,), jnp.float32), 0.1, 1.9)
    mixer_output_weight = centred(streams_of[7], (HEADS * VALUE_DIM, D), (HEADS * VALUE_DIM) ** -0.5, 0.125, ((0, 4),))
    expert_input_rows = centred(streams_of[8], (MOE_TOKENS, D), 1.0, 6.0, ((0, 256),))
    expert_norm_gain = jnp.clip(1.0 + 0.18 * jax.random.normal(streams_of[9], (D,), jnp.float32), 0.1, 1.9)
    routes_keys = jax.random.split(jax.random.fold_in(streams_of[10], 1), MOE_TOKENS // MOE_TOK)
    routes_turns = jax.random.permutation(jax.random.fold_in(streams_of[10], 3), MOE_TOKENS // MOE_TOK)
    routes = jax.vmap(lambda own, number: assign_block(jax.random.fold_in(streams_of[10], 2), own, number, MOE_TOK, EXPERTS, TOPK, CAP, 1))(routes_keys, routes_turns).reshape((MOE_TOKENS, TOPK))
    router_picked_scores = jnp.clip(jnp.exp(math.log(1.0) - 2.3025851 * jax.random.uniform(streams_of[11], (MOE_TOKENS, TOPK), jnp.float32) ** shard_levels(streams_of[11], (MOE_TOKENS, TOPK), ((0, 256),), -0.2, 0.2)), 0.1, 1.0)
    expert_gate_weight = centred(streams_of[12], (EXPERTS, D, EXPERT_HIDDEN), D ** -0.5, 0.125, ((0, 64), (2, 4)))
    expert_up_weight = centred(streams_of[13], (EXPERTS, D, EXPERT_HIDDEN), D ** -0.5, 0.125, ((0, 64), (2, 4)))
    expert_down_weight = centred(streams_of[14], (EXPERTS, D, EXPERT_HIDDEN), EXPERT_HIDDEN ** -0.5, 0.1875, ((0, 64), (2, 4)))
    return {"queries": queries, "mixer_key_rows": mixer_key_rows, "mixer_value_rows": mixer_value_rows, "log_input_gate": log_input_gate, "forget_gate_logits": forget_gate_logits, "extra_log_decay": extra_log_decay, "head_norm_gain": head_norm_gain, "mixer_output_weight": mixer_output_weight, "expert_input_rows": expert_input_rows, "expert_norm_gain": expert_norm_gain, "routes": routes, "router_picked_scores": router_picked_scores, "expert_gate_weight": expert_gate_weight, "expert_up_weight": expert_up_weight, "expert_down_weight": expert_down_weight}


EPSILON = 1e-06
LOW_LEVEL = -1e+30

def mixer_baseline(queries, mixer_key_rows, mixer_value_rows, log_input_gate, forget_gate_logits, extra_log_decay, head_norm_gain, mixer_output_weight):
    token_count = queries.shape[0]
    head_count = log_input_gate.shape[0]
    block_count = token_count // BLOCK
    query_scale = KEY_DIM ** (-0.5)

    def to_blocks(tensor, lane):
        return tensor.reshape(block_count, BLOCK, head_count, lane).transpose(0, 2, 1, 3)
    query_blocks = to_blocks(queries, KEY_DIM)
    key_blocks = to_blocks(mixer_key_rows, KEY_DIM)
    value_blocks = to_blocks(mixer_value_rows, VALUE_DIM)
    forget_log_value = jax.nn.log_sigmoid(forget_gate_logits) + extra_log_decay
    forget_blocks = forget_log_value.reshape(head_count, block_count, BLOCK).transpose(1, 0, 2)
    input_blocks = log_input_gate.reshape(head_count, block_count, BLOCK).transpose(1, 0, 2)
    causal_mask = jnp.tril(jnp.ones((BLOCK, BLOCK), dtype=bool))
    highest = lax.Precision.HIGHEST

    def advance(carry, inputs):
        memory, level_in = carry
        query_blk, key_blk, value_blk, input_blk, forget_blk = inputs
        query_f = query_blk.astype(jnp.float32) * query_scale
        key_f = key_blk.astype(jnp.float32)
        value_f = value_blk.astype(jnp.float32)
        cumulative = jnp.cumsum(forget_blk, axis=-1)
        span_decay = cumulative[:, -1]
        within = cumulative[:, :, None] - cumulative[:, None, :] + input_blk[:, None, :]
        within = jnp.where(causal_mask, within, -jnp.inf)
        carried = cumulative + level_in[:, None]
        row_max = jnp.maximum(carried, lax.optimization_barrier(jnp.max(within, axis=-1)))
        scores = jnp.einsum('hjd,hsd->hjs', query_f, key_f, precision=highest) * jnp.exp(within - row_max[..., None])
        cell = jnp.einsum('hjs,hse->hje', scores, value_f, precision=highest)
        cell = cell + jnp.exp(carried - row_max)[..., None] * jnp.einsum('hjd,hde->hje', query_f, memory, precision=highest)
        normed = cell * lax.rsqrt(lax.optimization_barrier(jnp.mean(cell * cell, axis=-1, keepdims=True)) + EPSILON)
        gap = span_decay[:, None] - cumulative + input_blk
        local_level = lax.optimization_barrier(jnp.max(gap, axis=-1))
        weighted = key_f * jnp.exp(gap - local_level[:, None])[..., None]
        local_memory = jnp.einsum('hsd,hse->hde', weighted, value_f, precision=highest)
        new_level = jnp.maximum(span_decay + level_in, local_level)
        memory = jnp.exp(span_decay + level_in - new_level)[:, None, None] * memory + jnp.exp(local_level - new_level)[:, None, None] * local_memory
        return ((memory, new_level), normed.transpose(1, 0, 2).reshape(BLOCK, head_count * VALUE_DIM))
    start = (jnp.zeros((head_count, KEY_DIM, VALUE_DIM), jnp.float32), jnp.full((head_count,), LOW_LEVEL, jnp.float32))
    _, normed = lax.scan(advance, start, (query_blocks, key_blocks, value_blocks, input_blocks, forget_blocks))
    normed = (normed.reshape(token_count, head_count * VALUE_DIM) * head_norm_gain).astype(jnp.bfloat16)
    group = head_count * VALUE_DIM // N_TP
    totals = jnp.zeros((token_count, mixer_output_weight.shape[1]), jnp.float32)
    for group_index in range(N_TP):
        columns = normed[:, group_index * group:(group_index + 1) * group]
        weight_rows = mixer_output_weight[group_index * group:(group_index + 1) * group]
        partial_value = jnp.dot(columns, weight_rows, preferred_element_type=jnp.float32).astype(jnp.bfloat16)
        totals = totals + partial_value.astype(jnp.float32)
    return totals.astype(jnp.bfloat16)

def experts_reference(expert_input_rows, expert_norm_gain, routes, router_picked_scores, expert_gate_weight, expert_up_weight, expert_down_weight):
    token_count, model_width = expert_input_rows.shape
    expert_count = expert_gate_weight.shape[0]
    pick_count = routes.shape[1]
    block_total = N_EP * N_TP
    inputs_f = expert_input_rows.astype(jnp.float32)
    normed = (inputs_f * lax.rsqrt(lax.optimization_barrier(jnp.mean(inputs_f * inputs_f, axis=-1, keepdims=True)) + EPSILON) * expert_norm_gain).astype(jnp.bfloat16)
    share = router_picked_scores / lax.optimization_barrier(jnp.sum(router_picked_scores, axis=-1, keepdims=True))
    chosen = routes.reshape(block_total, MOE_TOK * pick_count)
    onehot = (chosen[..., None] == jnp.arange(expert_count, dtype=jnp.int32)).astype(jnp.int32)
    before = lax.optimization_barrier(jnp.sum((jnp.cumsum(onehot, axis=1) - onehot) * onehot, axis=-1))
    slot_index = jnp.arange(block_total, dtype=jnp.int32)[:, None] * CAP + before
    row_owner = (jnp.arange(token_count * pick_count, dtype=jnp.int32) // pick_count).reshape(block_total, -1)
    slot_owner = jnp.full((expert_count, block_total * CAP), token_count, jnp.int32).at[chosen, slot_index].set(row_owner)
    slot_share = jnp.zeros((expert_count, block_total * CAP), jnp.float32).at[chosen, slot_index].set(share.reshape(block_total, -1))
    padded = jnp.concatenate([normed, jnp.zeros((1, model_width), jnp.bfloat16)], axis=0)

    def visit(totals, inputs):
        owner_row, share_row, gate_mat, up_mat, down_mat = inputs
        picked = padded[owner_row]
        gate_val = jnp.dot(picked, gate_mat, preferred_element_type=jnp.float32)
        up_val = jnp.dot(picked, up_mat, preferred_element_type=jnp.float32)
        hidden = (jax.nn.silu(gate_val) * up_val).astype(jnp.bfloat16)
        result = lax.dot_general(hidden, down_mat, (((1,), (1,)), ((), ())), preferred_element_type=jnp.float32).astype(jnp.bfloat16)
        return (totals.at[owner_row].add(share_row[:, None] * result.astype(jnp.float32)), None)
    totals = jnp.zeros((token_count + 1, model_width), jnp.float32)
    totals, _ = lax.scan(visit, totals, (slot_owner, slot_share, expert_gate_weight, expert_up_weight, expert_down_weight))
    return totals[:token_count].astype(jnp.bfloat16)

def reference(queries, mixer_key_rows, mixer_value_rows, log_input_gate, forget_gate_logits, extra_log_decay, head_norm_gain, mixer_output_weight, expert_input_rows, expert_norm_gain, routes, router_picked_scores, expert_gate_weight, expert_up_weight, expert_down_weight):
    mixer_output = mixer_baseline(queries, mixer_key_rows, mixer_value_rows, log_input_gate, forget_gate_logits, extra_log_decay, head_norm_gain, mixer_output_weight)
    expert_out = experts_reference(expert_input_rows, expert_norm_gain, routes, router_picked_scores, expert_gate_weight, expert_up_weight, expert_down_weight)
    return (mixer_output, expert_out)
```

```python
import jax
import jax.numpy as jnp
from jax import lax
from jax.experimental import pallas as pl
from jax.experimental.pallas import tpu as pltpu
from jax.sharding import Mesh
from jax.sharding import PartitionSpec as P


EP = ("ep_0", "ep_1", "ep_2")
EP_TP = ("ep_0", "ep_1", "ep_2", "tp")
EPSILON = 1e-06
LOW_LEVEL = -1e30
F32 = jnp.float32
BF16 = jnp.bfloat16

N_EP = 64
N_TP = 4
TOK = 512
KEY = 128
VAL = 256
WIDTH = 2048
QUARTER = 256
ROWS = 64
CAP = 6
PIECES = 8
PIECE = 256
MSG = CAP * PIECES
EXPERTS = 64
GROUP = 8
BLOCKS = 4
PART = WIDTH // BLOCKS

PARAMS = pltpu.CompilerParams(vmem_limit_bytes=56 * 1024 * 1024)
SMALL = pltpu.CompilerParams(vmem_limit_bytes=40 * 1024 * 1024)


def iota(shape, dim):
    return lax.broadcasted_iota(jnp.int32, shape, dim)


def dot(a, b):
    return jnp.dot(a, b, preferred_element_type=F32)


def dot_nt(a, b):
    return lax.dot_general(a, b, (((1,), (1,)), ((), ())), preferred_element_type=F32)


def in_vmem(x):
    return pltpu.with_memory_space_constraint(x, pltpu.VMEM)


def two_parts(x):
    high = x.astype(BF16).astype(F32)
    return high, (x - high).astype(BF16).astype(F32)


def three_parts(x):
    high = x.astype(BF16).astype(F32)
    rest = x - high
    middle = rest.astype(BF16).astype(F32)
    return high, middle, (rest - middle).astype(BF16).astype(F32)


def state_body(keys, values, gate_in, log_forget, state, gaps):
    upper = (iota((TOK, TOK), 0) <= iota((TOK, TOK), 1)).astype(F32).astype(BF16)
    odd = (iota((8, TOK), 0) & 1) == 1
    decay = jnp.where(odd, log_forget[1:2], log_forget[0:1])
    parts = jnp.concatenate(three_parts(decay), axis=0).astype(BF16)
    sums = dot(parts, upper)
    total = sums[0:8] + sums[8:16] + sums[16:24]
    gap = jnp.where(odd, gate_in[1:2], gate_in[0:1]) - total
    gaps[...] = gap
    blocks = []
    lane = iota((8, 128), 1)
    row = iota((8, 128), 0)
    scalars = jnp.zeros((8, 128), F32)
    for h in range(2):
        own = gap[h : h + 1]
        highest = jnp.max(own, axis=1, keepdims=True)
        key_t = keys[:, h * KEY : (h + 1) * KEY].astype(F32).T
        weighted = key_t * jnp.exp(own - highest)
        own_values = values[:, h * VAL : (h + 1) * VAL]
        memory = sum(dot(part.astype(BF16), own_values) for part in two_parts(weighted))
        blocks += [memory[:, :128], memory[:, 128:]]
        for n, part in enumerate(three_parts(highest) + three_parts(total[h : h + 1, TOK - 1 : TOK])):
            scalars = scalars + jnp.where((lane == 6 * h + n) & (row == 0), part, 0.0)
    stacked = jnp.concatenate(blocks, axis=0).reshape(N_EP, 8, 128)
    spread = jnp.broadcast_to(scalars[None], (N_EP, 8, 128))
    high, low = two_parts(stacked)
    upper_rows = jnp.concatenate([high, spread], axis=2)
    lower_rows = jnp.concatenate([low, jnp.zeros_like(spread)], axis=2)
    state[...] = jnp.concatenate([upper_rows, lower_rows], axis=1).astype(BF16)


def prefix_body(index, arrived, prefix, level):
    place = index[0]
    full = arrived[:, MSG:, :].astype(F32)
    high = full[:, :8, :128].reshape(N_EP * 8, 128).astype(BF16)
    low = full[:, 8:, :128].reshape(N_EP * 8, 128).astype(BF16)
    scalars = jnp.sum(full[:, :8, 128:], axis=1)
    row, col = iota((N_EP, N_EP), 0), iota((N_EP, N_EP), 1)
    earlier = col < row
    factors = []
    own_row = iota((N_EP, 1), 0) == place
    out_row = iota((8, 128), 0)
    levels = jnp.zeros((8, 128), F32)
    for h in range(2):
        cols = [scalars[:, 6 * h + n : 6 * h + n + 1] for n in range(6)]
        highest = cols[0] + cols[1] + cols[2]
        decay = cols[3] + cols[4] + cols[5]
        highest_row = jnp.sum(jnp.where(row == col, highest, 0.0), axis=0, keepdims=True)
        between = jnp.dot(
            earlier.astype(F32),
            jnp.where(row >= col, decay, 0.0),
            precision=lax.Precision.HIGHEST,
            preferred_element_type=F32,
        )
        exponent = jnp.where(earlier, highest_row + between, -3e38)
        top = jnp.maximum(jnp.max(exponent, axis=1, keepdims=True), LOW_LEVEL)
        factors.append(jnp.where(earlier, jnp.exp(exponent - top), 0.0))
        mine = jnp.sum(jnp.where(own_row, top, 0.0), axis=0, keepdims=True)
        levels = levels + jnp.where(out_row == h, mine, 0.0)
    level[...] = levels
    factor = jnp.where(place >= N_EP // 2, factors[1], factors[0]).astype(BF16)
    wide = N_EP * 8
    spread = ((iota((wide, N_EP), 0) >> 3) == iota((wide, N_EP), 1)).astype(F32).astype(BF16)
    spread_t = (iota((N_EP, wide), 0) == (iota((N_EP, wide), 1) >> 3)).astype(F32).astype(BF16)
    repeated = dot(dot(spread, factor).astype(BF16), spread_t)
    same = (iota((wide, wide), 0) & 7) == (iota((wide, wide), 1) & 7)
    mixing = jnp.where(same, repeated, 0.0).astype(BF16)
    mixed = (dot(mixing, high) + dot(mixing, low)).reshape(N_EP, 8, 128)
    prefix[...] = jnp.concatenate(two_parts(mixed), axis=1).astype(BF16)


def cell_body(index, queries, keys, values, gaps, prefix, level, gain, weight, out_0, out_1, out_2, out_3, normed, partial):
    slices = prefix[...].astype(F32)
    halves = [slices[:, :8].reshape(N_EP * 8, 128), slices[:, 8:].reshape(N_EP * 8, 128)]
    causal = iota((TOK, TOK), 1) <= iota((TOK, TOK), 0)
    for h in range(2):
        query = queries[:, h * KEY : (h + 1) * KEY]
        recalled = 0.0
        for part in halves:
            columns = [part[256 * h : 256 * h + 128], part[256 * h + 128 : 256 * h + 256]]
            recalled = recalled + dot(query, jnp.concatenate(columns, axis=1).astype(BF16))
        exponent = jnp.where(causal, gaps[h : h + 1, :], -jnp.inf)
        carried = level[h : h + 1, 0:1]
        top = jnp.maximum(jnp.max(exponent, axis=1, keepdims=True), carried)
        scores = dot_nt(query, keys[:, h * KEY : (h + 1) * KEY]) * (KEY**-0.5)
        scores = scores * jnp.exp(exponent - top)
        cell = dot(scores.astype(BF16), values[:, h * VAL : (h + 1) * VAL])
        cell = cell + (jnp.exp(carried - top) * KEY**-0.5) * recalled
        scale = lax.rsqrt(jnp.mean(cell * cell, axis=1, keepdims=True) + EPSILON)
        normed[:, h * VAL : (h + 1) * VAL] = (cell * scale * gain[:, h * VAL : (h + 1) * VAL]).astype(BF16)
    for c in range(0, WIDTH, 512):
        partial[:, c : c + 512] = dot(normed[...], weight[:, c : c + 512]).astype(BF16)
    for n, out in enumerate((out_0, out_1, out_2, out_3)):
        first = pl.multiple_of(lax.rem(index[0] + n, N_TP) * 128, 128)
        out[...] = partial[pl.ds(first, 128), :]


def mixer_state(keys, values, log_input_gate, forget_gate_logits, extra_log_decay):
    log_forget = jax.nn.log_sigmoid(forget_gate_logits) + extra_log_decay
    return pl.pallas_call(
        state_body,
        out_shape=(
            jax.ShapeDtypeStruct((N_EP, 16, PIECE), BF16),
            jax.ShapeDtypeStruct((8, TOK), F32),
        ),
        compiler_params=PARAMS,
        name="local_state",
    )(keys, values, log_input_gate, log_forget)


def mixer_prefix(index, arrived):
    return pl.pallas_call(
        prefix_body,
        in_specs=[
            pl.BlockSpec(memory_space=pltpu.SMEM),
            pl.BlockSpec(memory_space=pltpu.VMEM),
        ],
        out_shape=(
            jax.ShapeDtypeStruct((N_EP, 16, 128), BF16),
            jax.ShapeDtypeStruct((8, 128), F32),
        ),
        compiler_params=PARAMS,
        name="prefix",
    )(index, in_vmem(arrived))


def mixer_cells(index, queries, keys, values, gaps, prefix, level, gain, weight):
    vmem = pl.BlockSpec(memory_space=pltpu.VMEM)
    return pl.pallas_call(
        cell_body,
        in_specs=[pl.BlockSpec(memory_space=pltpu.SMEM)] + [vmem] * 8,
        out_specs=[vmem] * 4,
        out_shape=[jax.ShapeDtypeStruct((128, WIDTH), BF16)] * 4,
        scratch_shapes=[pltpu.VMEM((TOK, 2 * VAL), BF16), pltpu.VMEM((TOK, WIDTH), BF16)],
        compiler_params=PARAMS,
        name="cells",
    )(index, queries, keys, values, gaps, in_vmem(prefix), level, gain.reshape(1, -1), weight)


def dispatch_body(rows, gain, routes, scores, state, outgoing, select, stacked, slots):
    inputs = rows[...].astype(F32)
    scale = lax.rsqrt(jnp.mean(inputs * inputs, axis=1, keepdims=True) + EPSILON)
    normed = (inputs * scale * gain[...]).astype(BF16)
    for c in range(PIECES):
        stacked[c * ROWS : (c + 1) * ROWS, :] = normed[:, c * PIECE : (c + 1) * PIECE]
    expert = iota((EXPERTS, ROWS), 0)
    hits = [routes[p : p + 1] == expert for p in range(3)]
    named = hits[0] | hits[1] | hits[2]
    before = (iota((ROWS, ROWS), 0) < iota((ROWS, ROWS), 1)).astype(F32).astype(BF16)
    rank = dot(named.astype(F32).astype(BF16), before)
    place = jnp.where(named, rank, -1.0).astype(BF16)
    share = scores[...] / jnp.sum(scores[...], axis=0, keepdims=True)
    shares = sum(jnp.where(hits[p], share[p : p + 1], 0.0) for p in range(3)).astype(BF16)
    wide = PIECES * ROWS
    repeat = (iota((ROWS, wide), 0) == (iota((ROWS, wide), 1) & (ROWS - 1))).astype(F32).astype(BF16)
    slots[...] = dot(place, repeat)
    row, col = iota((MSG, wide), 0), iota((MSG, wide), 1)
    piece = sum((row >= n * CAP).astype(jnp.int32) for n in range(1, PIECES))
    pattern = jnp.where((col >> 6) == piece, row - CAP * piece, -7).astype(F32)

    def one_group(g, carry):
        picks = []
        for e in range(GROUP):
            mine = slots[pl.ds(g * GROUP + e, 1), :]
            picks.append((jnp.broadcast_to(mine, (MSG, wide)) == pattern).astype(F32).astype(BF16))
        picked = dot(jnp.concatenate(picks, axis=0), stacked[...]).reshape(GROUP, MSG, PIECE)
        extra = state[pl.ds(g * GROUP, GROUP)].astype(F32)
        outgoing[pl.ds(g * GROUP, GROUP)] = jnp.concatenate([picked, extra], axis=1).astype(BF16)
        return carry

    lax.fori_loop(0, EXPERTS // GROUP, one_group, 0)
    same = (iota((ROWS, ROWS), 0) == iota((ROWS, ROWS), 1)).astype(F32).astype(BF16)
    spread, slot, _ = message_columns()
    long_place = dot(dot_nt(same, place).astype(BF16), spread)
    long_share = dot(dot_nt(same, shares).astype(BF16), spread)
    select[...] = jnp.where(long_place == slot, long_share, 0.0).astype(BF16)


def message_columns():
    long = EXPERTS * MSG
    offset = iota((EXPERTS, long), 1) - iota((EXPERTS, long), 0) * MSG
    inside = (offset >= 0) & (offset < MSG)
    within = jnp.sum(jnp.where(inside, offset.astype(F32), 0.0), axis=0, keepdims=True)
    piece = sum((within >= n * CAP).astype(F32) for n in range(1, PIECES))
    return inside.astype(F32).astype(BF16), within - CAP * piece, piece


def turn_matrix(pieces, back):
    size = GROUP * CAP * pieces
    own, other = (1, 0) if back else (0, 1)
    line = iota((1, size) if back else (size, 1), own)
    piece = sum((line >= n * MSG).astype(jnp.int32) for n in range(1, pieces))
    line = line - MSG * piece
    source = sum((line >= n * CAP).astype(jnp.int32) for n in range(1, GROUP))
    place = source * (CAP * pieces) + piece * CAP + line - CAP * source
    return (iota((size, size), other) == place).astype(F32).astype(BF16)


def gated(rows, both):
    products = dot(rows, both)
    return (jax.nn.silu(products[:, :QUARTER]) * products[:, QUARTER:]).astype(BF16)


def hidden_near_body(arrived, *refs):
    weights, (hidden, rows, loaded, done) = refs[:6], refs[6:]
    copies = []
    for n, weight in enumerate(weights):
        lanes = pl.ds((n % 2) * QUARTER, QUARTER)
        copies.append(pltpu.make_async_copy(weight, loaded.at[n // 2, :, lanes], done.at[n]))
    for copy in copies:
        copy.start()
    order = turn_matrix(PIECES, False)
    for g in range(N_EP // GROUP):
        block = arrived[g * GROUP : (g + 1) * GROUP, :MSG].reshape(GROUP * MSG, PIECE)
        turned = dot(order, block).astype(BF16)
        for c in range(PIECES):
            rows[g * MSG : (g + 1) * MSG, c * PIECE : (c + 1) * PIECE] = turned[c * MSG : (c + 1) * MSG]
    for q in range(3):
        copies[2 * q].wait()
        copies[2 * q + 1].wait()
        hidden[:, q * QUARTER : (q + 1) * QUARTER] = gated(rows[...], loaded[q])


def hidden_far_body(rows, gate, up, hidden):
    hidden[...] = gated(rows[...], jnp.concatenate([gate[...], up[...]], axis=1))


def down_near_body(hidden, out, *refs):
    ups_of, downs_of = refs[:BLOCKS], refs[BLOCKS : 2 * BLOCKS]
    partial_low, partial_high, loaded, done = refs[2 * BLOCKS :]
    copies = []
    for n in range(BLOCKS):
        rows = pl.ds(n * PART, PART)
        for q, source in enumerate((out.at[rows], ups_of[n], downs_of[n])):
            target = loaded.at[rows, pl.ds(q * QUARTER, QUARTER)]
            copies.append(pltpu.make_async_copy(source, target, done.at[3 * n + q]))
    for copy in copies:
        copy.start()
    half = WIDTH // 2
    for part, partial in enumerate((partial_low, partial_high)):
        for copy in copies[6 * part : 6 * part + 6]:
            copy.wait()
        partial[...] = dot_nt(hidden[...], loaded[part * half : (part + 1) * half, :])


def far_messages(hidden, partial, w_a, w_b, result, lines):
    order = turn_matrix(PIECES // 2, True)
    far = jnp.concatenate([dot_nt(hidden[...], w_a[...]), dot_nt(hidden[...], w_b[...])], axis=1)
    total = (partial[...] + far).astype(BF16)
    for g in range(N_EP // GROUP):
        block = total[g * MSG : (g + 1) * MSG]
        pieces = [block[:, c * PIECE : (c + 1) * PIECE] for c in range(PIECES // 2)]
        turned = dot(order, jnp.concatenate(pieces, axis=0)).astype(BF16)
        result[g * GROUP : (g + 1) * GROUP, lines] = turned.reshape(GROUP, MSG // 2, PIECE)


def down_low_body(hidden, partial, w_a, w_b, result):
    far_messages(hidden, partial, w_a, w_b, result, slice(0, MSG // 2))


def down_high_body(hidden, partial, w_a, w_b, low, result):
    result[:, : MSG // 2] = low[...]
    far_messages(hidden, partial, w_a, w_b, result, slice(MSG // 2, MSG))


def spread_body(select, shares):
    _, _, piece = message_columns()
    base = select[...].astype(F32)
    for c in range(PIECES):
        shares[c * ROWS : (c + 1) * ROWS, :] = jnp.where(piece == c, base, 0.0).astype(BF16)


def combine_body(shares, returned, out):
    long = EXPERTS * MSG
    rows = returned[...].reshape(long, PIECE)
    middle = long // 2
    total = dot(shares[:, :middle], rows[:middle]) + dot(shares[:, middle:], rows[middle:])
    total = total.astype(BF16)
    for c in range(PIECES):
        out[:, c * PIECE : (c + 1) * PIECE] = total[c * ROWS : (c + 1) * ROWS]


def dispatch(rows, gain, routes, scores, state):
    return pl.pallas_call(
        dispatch_body,
        out_shape=(
            jax.ShapeDtypeStruct((EXPERTS, MSG + 16, PIECE), BF16),
            jax.ShapeDtypeStruct((ROWS, EXPERTS * MSG), BF16),
        ),
        scratch_shapes=[
            pltpu.VMEM((PIECES * ROWS, PIECE), BF16),
            pltpu.VMEM((EXPERTS, PIECES * ROWS), F32),
        ],
        compiler_params=PARAMS,
        name="dispatch",
    )(rows, gain.reshape(1, -1), routes.T, scores.T, state)


def hidden_near(arrived, weights):
    vmem = pl.BlockSpec(memory_space=pltpu.VMEM)
    anywhere = pl.BlockSpec(memory_space=pl.ANY)
    return pl.pallas_call(
        hidden_near_body,
        in_specs=[vmem] + [anywhere] * 6,
        out_specs=(vmem, vmem),
        out_shape=(
            pltpu.VMEM((N_EP * CAP, 3 * QUARTER), BF16),
            jax.ShapeDtypeStruct((N_EP * CAP, WIDTH), BF16),
        ),
        scratch_shapes=[
            pltpu.VMEM((3, WIDTH, 2 * QUARTER), BF16),
            pltpu.SemaphoreType.DMA((6,)),
        ],
        compiler_params=PARAMS,
        name="hidden_near",
    )(in_vmem(arrived), *weights)


def hidden_far(rows, gate, up):
    vmem = pl.BlockSpec(memory_space=pltpu.VMEM)
    return pl.pallas_call(
        hidden_far_body,
        in_specs=[vmem] * 3,
        out_specs=vmem,
        out_shape=pltpu.VMEM((N_EP * CAP, QUARTER), BF16),
        compiler_params=SMALL,
        name="hidden_far",
    )(rows, in_vmem(gate), in_vmem(up))


def down_near(hidden, out, ups_of, downs_of):
    vmem = pl.BlockSpec(memory_space=pltpu.VMEM)
    anywhere = pl.BlockSpec(memory_space=pl.ANY)
    return pl.pallas_call(
        down_near_body,
        in_specs=[vmem] + [anywhere] * (1 + 2 * BLOCKS),
        out_specs=(vmem, vmem),
        out_shape=(pltpu.VMEM((N_EP * CAP, WIDTH // 2), F32),) * 2,
        scratch_shapes=[
            pltpu.VMEM((WIDTH, 3 * QUARTER), BF16),
            pltpu.SemaphoreType.DMA((3 * BLOCKS,)),
        ],
        compiler_params=PARAMS,
        name="down_near",
    )(in_vmem(hidden), out, *ups_of, *downs_of)


def down_far(body, lines, *operands):
    vmem = pl.BlockSpec(memory_space=pltpu.VMEM)
    return pl.pallas_call(
        body,
        in_specs=[vmem] * len(operands),
        out_specs=vmem,
        out_shape=pltpu.VMEM((N_EP, lines, PIECE), BF16),
        compiler_params=SMALL,
        name="down_far",
    )(*[in_vmem(x) for x in operands])


def spread_shares(select):
    vmem = pl.BlockSpec(memory_space=pltpu.VMEM)
    return pl.pallas_call(
        spread_body,
        in_specs=[vmem],
        out_specs=vmem,
        out_shape=pltpu.VMEM((PIECES * ROWS, EXPERTS * MSG), BF16),
        compiler_params=SMALL,
        name="spread",
    )(select)


def combine(shares, returned):
    return pl.pallas_call(
        combine_body,
        out_shape=jax.ShapeDtypeStruct((ROWS, WIDTH), BF16),
        compiler_params=SMALL,
        name="combine",
    )(in_vmem(shares), in_vmem(returned))


UP = [(i, (i + 1) % N_TP) for i in range(N_TP)]
DOWN = [(i, (i - 1) % N_TP) for i in range(N_TP)]
ACROSS = [(i, (i + 2) % N_TP) for i in range(N_TP)]


def send(x, ring):
    return lax.ppermute(x, "tp", ring)


def exchange(x):
    return lax.all_to_all(x, EP, split_axis=0, concat_axis=0, tiled=True)


def shards(
    queries,
    mixer_key_rows,
    mixer_value_rows,
    log_input_gate,
    forget_gate_logits,
    extra_log_decay,
    head_norm_gain,
    mixer_output_weight,
    expert_input_rows,
    expert_norm_gain,
    routes,
    router_picked_scores,
    expert_gate_weight,
    expert_up_weight,
    expert_down_weight,
):
    ep_index = lax.axis_index(EP).astype(jnp.int32).reshape(1)
    tp_index = lax.axis_index("tp").astype(jnp.int32).reshape(1)
    gate, up, out = expert_gate_weight[0], expert_up_weight[0], expert_down_weight[0]

    gates = [gate, send(gate, UP), send(gate, DOWN)]
    ups = [up, send(up, UP), send(up, DOWN)]
    gates.append(send(gates[1], UP))
    ups.append(send(ups[2], DOWN))
    ups_of, downs_of = [], []
    for n in range(BLOCKS):
        block = out[n * PART : (n + 1) * PART]
        ups_of.append(send(block, UP))
        downs_of.append(send(block, DOWN))
    far_outs = [send(downs_of[n], DOWN) if n % 2 else send(ups_of[n], UP) for n in range(BLOCKS)]

    state, gaps = mixer_state(
        mixer_key_rows, mixer_value_rows, log_input_gate, forget_gate_logits, extra_log_decay
    )
    outgoing, select = dispatch(
        expert_input_rows, expert_norm_gain, routes, router_picked_scores, state
    )
    arrived = exchange(outgoing)
    slices, level = mixer_prefix(ep_index, arrived)
    prefix = exchange(slices)

    near = [w for pair in zip(gates[:3], ups[:3]) for w in pair]
    near_units, rows = hidden_near(arrived, near)
    far_units = hidden_far(rows, gates[3], ups[3])

    own, to_up, to_across, to_down = mixer_cells(
        tp_index,
        queries,
        mixer_key_rows,
        mixer_value_rows,
        gaps,
        prefix,
        level,
        head_norm_gain,
        mixer_output_weight,
    )
    parts = [own, send(to_up, UP), send(to_across, ACROSS), send(to_down, DOWN)]

    partial_low, partial_high = down_near(near_units, out, ups_of, downs_of)
    low = down_far(down_low_body, MSG // 2, far_units, partial_low, *far_outs[:2])
    result = down_far(down_high_body, MSG, far_units, partial_high, *far_outs[2:], low)
    returned = exchange(result)
    mixer_output = sum(part.astype(F32) for part in parts).astype(BF16)
    shares = spread_shares(select)
    expert_out = combine(shares, returned)
    return (mixer_output, expert_out)


def solution(mesh):
    split = Mesh(mesh.devices.reshape(8, 4, 2, mesh.shape["tp"]), EP_TP)
    in_specs = (
        P(EP, "tp"),
        P(EP, "tp"),
        P(EP, "tp"),
        P("tp", EP),
        P("tp", EP),
        P("tp", EP),
        P("tp"),
        P("tp", None),
        P(EP_TP, None),
        P(),
        P(EP_TP, None),
        P(EP_TP, None),
        P(EP, None, "tp"),
        P(EP, None, "tp"),
        P(EP, None, "tp"),
    )
    out_specs = (P(EP_TP, None), P(EP_TP, None))

    return jax.shard_map(
        shards, mesh=split, in_specs=in_specs, out_specs=out_specs, check_vma=False
    )
```
